32 devices in a mesh: sp: 8 (over z, x), dp: 4 (over y, core).
Axes of the slice: x: 2, y: 2, z: 4, core: 2. Of those that a mesh axis runs over, the one named last changes fastest.
Arguments:
- resid: bfloat16 [4, 1024, 2048], P('dp', 'sp'), may hold values from -6 to 6
- queries: bfloat16 [4, 1024, 2048], P('dp', 'sp'), may hold values from -7 to 7
- keys: bfloat16 [4, 1024, 2048], P('dp', 'sp'), may hold values from -7 to 7
- values: bfloat16 [4, 1024, 2048], P('dp', 'sp'), may hold values from -6 to 6
- forget_cache: float32 [4, 32, 1024], P('dp', 'sp'), may hold values from -131 to 0, as said below
- query_gain: float32 [64], replicated, may hold values from 0.5 to 8
- key_gain: float32 [64], replicated, may hold values from 0.5 to 8
- out_weight: bfloat16 [2048, 2048], P(None, 'dp'), may hold values from -0.125 to 0.125
- norm_gain: float32 [2048], replicated, may hold values from 0.1 to 1.9
- routes: int32 [4, 1024, 2], P('dp', 'sp'), may hold values from 0 to 31, all different within a row; in each aligned block of 128 rows (0 to 127, 128 to 255, ..., all dimensions but the last counted through in order) at most 16 rows name the same one
- group_weight: float32 [4, 1024], P('dp', 'sp'), may hold values from 0.2 to 1
- inner_share: float32 [4, 1024, 2], P('dp', 'sp'), may hold values from 0.1 to 1
- expert_gate: bfloat16 [32, 2048, 1024], P(('sp', 'dp')), may hold values from -0.125 to 0.125
- expert_up: bfloat16 [32, 2048, 1024], P(('sp', 'dp')), may hold values from -0.125 to 0.125
- expert_down: bfloat16 [32, 1024, 2048], P(('sp', 'dp')), may hold values from -0.1875 to 0.1875
Outputs:
- layer_out: bfloat16 [4, 1024, 2048], P('dp', 'sp')
The draws below stay inside these ranges and needn't reach their ends.
Inputs may be any that keep to these rules, and one draw needn't show every extreme that they name: `routes`: each row names 2 different experts; the rows of one device name one expert at most 16 times, a bound that some block reaches. `forget_cache`: along positions each head's values never rise.
All inputs are finite; a program needn't handle non-finite values.
Results may differ from the reference program's by a relative error of at most 0.0095.
The reference program's roundings to bfloat16 on the way count: a program that leaves them out, or rounds other values in their place, can miss the bound.
Values may be sent and summed in bfloat16 or wider, within the bound.
No kernel may reach another device: no remote copies, remote signals or barrier semaphores. Data moves between devices by JAX's collectives and lax.ppermute only.
A program may use at most 128 MiB of HBM per device.

```python
import math
import jax
import jax.numpy as jnp
import numpy as np
from jax import lax

D = 2048
HEAD_COUNT = 32
HD = 64
FF = 1024
TOPK = 2
TOK_DEV = 128
SEQUENCE_COUNT = 4
SEQUENCE_LENGTH = 1024
EXPERTS = 32
CAP = 16


def paired_rows(key):
    base = jax.random.fold_in(key, 7)
    key_q, key_k = jax.random.split(base, 2)
    shape = (SEQUENCE_COUNT, SEQUENCE_LENGTH, HEAD_COUNT * HD)
    key_rows = jax.random.truncated_normal(key_k, -6.0, 6.0, shape, jnp.float32)
    query_rows = jax.random.truncated_normal(key_q, -6.0, 6.0, shape, jnp.float32)
    return (query_rows, key_rows)


def draw_queries(key, part):
    return paired_rows(key)[0].astype(jnp.bfloat16)


def draw_keys(key, part):
    return paired_rows(key)[1].astype(jnp.bfloat16)


def draw_query_gain(key, part):
    sub = jax.random.fold_in(key, 11)
    return jax.random.uniform(sub, (HD,), jnp.float32, 0.5, 1.5)


def draw_key_gain(key, part):
    sub = jax.random.fold_in(key, 13)
    return jax.random.uniform(sub, (HD,), jnp.float32, 0.5, 1.5)


def draw_forget_cache(key, part):
    random_keys = jax.random.split(jax.random.fold_in(key, 17), 7)
    order = jax.random.permutation(random_keys[0], HEAD_COUNT)
    slow = order < HEAD_COUNT // 2
    total = jax.random.uniform(random_keys[1], (SEQUENCE_COUNT, HEAD_COUNT), jnp.float32, 0.3, 1.0)
    fast_span = jax.random.uniform(random_keys[2], (SEQUENCE_COUNT, HEAD_COUNT), jnp.float32, 30.0, 100.0)
    rate = jnp.where(slow[None, :], total / SEQUENCE_LENGTH, 1.0 / fast_span)
    blocks = SEQUENCE_LENGTH // TOK_DEV
    factor = jnp.exp(jax.random.uniform(random_keys[3], (SEQUENCE_COUNT, HEAD_COUNT, blocks), jnp.float32, -0.693, 0.693))
    factor = jnp.repeat(factor, TOK_DEV, axis=2)
    rough = jax.random.uniform(random_keys[4], (SEQUENCE_COUNT, HEAD_COUNT, SEQUENCE_LENGTH), jnp.float32, 0.3, 1.7)
    baseline_level = -rate[:, :, None] * factor * rough
    spike_location = jax.random.randint(random_keys[5], (SEQUENCE_COUNT, HEAD_COUNT, 3), 0, SEQUENCE_LENGTH)
    spike_dropped = jnp.log(jax.random.uniform(random_keys[6], (SEQUENCE_COUNT, HEAD_COUNT, 3), jnp.float32, 0.5, 0.8))
    token_offset = jnp.arange(SEQUENCE_LENGTH, dtype=jnp.int32)
    spike_events = jnp.sum(jnp.where(token_offset[None, None, None, :] == spike_location[..., None], spike_dropped[..., None], 0.0), axis=2)
    return jnp.cumsum(baseline_level + spike_events, axis=2)


def level_of(own_key, dims, cuts, smallest, top_value):
    def one(dim, parts):
        heights = jax.random.uniform(jax.random.fold_in(jax.random.fold_in(own_key, 6), dim), (parts,), jnp.float32, smallest / len(cuts), top_value / len(cuts))
        return jnp.repeat(jnp.exp(heights), dims[dim] // parts).reshape((-1,) + (1,) * (len(dims) - dim - 1))

    level = one(*cuts[0])
    for cut in cuts[1:]:
        level = level * one(*cut)
    return level


def shared_out(key, own, number, rows, count, top, bound, lean):
    ranking = jax.random.permutation(key, count)
    packed, ordinary = portions_of(count, rows * top, bound, lean, True), portions_of(count, rows * top, bound, lean, False)
    places = jnp.arange(count)

    def named(tallies, offset_by):
        used = int((tallies > 0).sum())
        fixed = max(1, used // 4)
        moved = fixed + (places - fixed + offset_by * (used - fixed)) % max(1, count - fixed)
        return jnp.zeros((count,), jnp.int32).at[ranking[jnp.where(places < fixed, places, moved)]].set(jnp.asarray(tallies, jnp.int32))

    tallies = jnp.where(number % 4 == 0, named(packed, number // 4), named(ordinary, number - number // 4 - 1))
    mixed = jax.random.permutation(jax.random.fold_in(own, 3), count)
    source_of, receiver = mixed[0:count // 2 * 2:2], mixed[1:count // 2 * 2:2]
    margin = jnp.minimum(tallies[source_of] - 1, bound - tallies[receiver]) // 2
    margin = jnp.where((source_of == ranking[0]) | (receiver == ranking[0]) | (tallies[receiver] == 0), 0, jnp.maximum(margin, 0))
    moved = jax.random.randint(jax.random.fold_in(own, 4), (count // 2,), 0, 1 << 20) % (margin + 1)
    tallies = tallies.at[source_of].add(-moved).at[receiver].add(moved)
    members = jnp.searchsorted(jnp.cumsum(tallies), jnp.arange(rows * top), side="right").astype(jnp.int32)
    listing = members.reshape(top, rows).T
    listing = listing[jax.random.permutation(jax.random.fold_in(own, 1), rows)]
    offset_by = jax.random.randint(jax.random.fold_in(own, 2), (rows, 1), 0, top)
    return jnp.take_along_axis(listing, (jnp.arange(top)[None, :] + offset_by) % top, axis=1)


def portions_of(number_of, total, limit, lean, full):
    loads = [(1 << 20) // math.isqrt(grade ** lean) + 1 for grade in range(1, number_of + 1)]
    largest = limit if full else min(limit, max(-(-total // number_of), total * loads[0] // sum(loads)))
    least = 1 if total - largest >= number_of - 1 else 0
    counts, surplus = [largest] + [least] * (number_of - 1), total - largest - least * (number_of - 1)
    while surplus > 0:
        free = [i for i in range(1, number_of) if counts[i] < largest] or [i for i in range(1, number_of) if counts[i] < limit]
        pool, remaining = sum([loads[i] for i in free]), surplus
        for i in free:
            extra = min(limit - counts[i], max(1, remaining * loads[i] // pool), surplus)
            counts[i] = counts[i] + extra
            surplus = surplus - extra
    return np.array(counts)


def centred(key, dims, width, limit, shards=(), kind=jnp.bfloat16):
    entries = jax.random.normal(key, dims, jnp.float32) * width
    if len(shards) > 0:
        entries = level_of(key, dims, shards, -0.22, 0.18) * entries
    return jnp.clip(entries, min=-limit, max=limit).astype(kind)


def setup_inputs(seed: int = 0) -> dict:
    key_of = jax.random.split(jax.random.key(seed), 16)
    resid = centred(key_of[0], (SEQUENCE_COUNT, SEQUENCE_LENGTH, D), 1.0, 6.0, ((0, 4), (1, 8)))
    queries = draw_queries(jax.random.fold_in(key_of[15], 71), 0)
    keys = draw_keys(jax.random.fold_in(key_of[15], 71), 0)
    values = centred(key_of[3], (SEQUENCE_COUNT, SEQUENCE_LENGTH, HEAD_COUNT * HD), 1.0, 6.0, ((0, 4), (1, 8)))
    forget_cache = draw_forget_cache(jax.random.fold_in(key_of[15], 71), 0)
    query_gain = draw_query_gain(jax.random.fold_in(key_of[15], 71), 0)
    key_gain = draw_key_gain(jax.random.fold_in(key_of[15], 71), 0)
    out_weight = centred(key_of[7], (HEAD_COUNT * HD, D), (HEAD_COUNT * HD) ** -0.5, 0.125, ((1, 4),))
    norm_gain = jnp.clip(1.0 + 0.18 * jax.random.normal(key_of[8], (D,), jnp.float32), 0.1, 1.9)
    routes_keys = jax.random.split(jax.random.fold_in(key_of[9], 1), SEQUENCE_COUNT * SEQUENCE_LENGTH // TOK_DEV)
    routes_turns = jax.random.permutation(jax.random.fold_in(key_of[9], 3), SEQUENCE_COUNT * SEQUENCE_LENGTH // TOK_DEV)
    routes = jax.vmap(lambda own, number: shared_out(jax.random.fold_in(key_of[9], 2), own, number, TOK_DEV, EXPERTS, TOPK, CAP, 2))(routes_keys, routes_turns).reshape((SEQUENCE_COUNT, SEQUENCE_LENGTH, TOPK))
    group_weight = jnp.clip(jnp.exp(math.log(1.0) - 1.609438 * jax.random.uniform(key_of[10], (SEQUENCE_COUNT, SEQUENCE_LENGTH), jnp.float32) ** level_of(key_of[10], (SEQUENCE_COUNT, SEQUENCE_LENGTH), ((0, 4), (1, 8)), -0.2, 0.2)), 0.2, 1.0)
    inner_share = jnp.clip(jnp.exp(math.log(1.0) - 2.3025851 * jax.random.uniform(key_of[11], (SEQUENCE_COUNT, SEQUENCE_LENGTH, TOPK), jnp.float32) ** level_of(key_of[11], (SEQUENCE_COUNT, SEQUENCE_LENGTH, TOPK), ((0, 4), (1, 8)), -0.2, 0.2)), 0.1, 1.0)
    expert_gate = centred(key_of[12], (EXPERTS, D, FF), D ** -0.5, 0.125, ((0, 32),))
    expert_up = centred(key_of[13], (EXPERTS, D, FF), D ** -0.5, 0.125, ((0, 32),))
    expert_down = centred(key_of[14], (EXPERTS, FF, D), FF ** -0.5, 0.1875, ((0, 32),))
    return dict(resid=resid, queries=queries, keys=keys, values=values, forget_cache=forget_cache, query_gain=query_gain, key_gain=key_gain, out_weight=out_weight, norm_gain=norm_gain, routes=routes, group_weight=group_weight, inner_share=inner_share, expert_gate=expert_gate, expert_up=expert_up, expert_down=expert_down)


EPS = 1e-06

def norm_rows(inputs, gain):
    floats = inputs.astype(jnp.float32)
    scaled = floats * lax.rsqrt(lax.optimization_barrier(jnp.mean(floats * floats, axis=-1, keepdims=True)) + EPS)
    return (scaled * gain.astype(jnp.float32)).astype(jnp.bfloat16)

def head_attention(operands):
    query_rows, key_rows, value_rows, decay = operands
    scores = jnp.dot(query_rows, key_rows.T, preferred_element_type=jnp.float32) * HD ** (-0.5)
    scores = scores + decay[:, None] - decay[None, :]
    token_offset = jnp.arange(query_rows.shape[0], dtype=jnp.int32)
    scores = jnp.where(token_offset[None, :] <= token_offset[:, None], scores, -jnp.inf)
    highest = lax.optimization_barrier(jnp.max(scores, axis=-1, keepdims=True))
    expd = jnp.exp(scores - highest)
    probs = (expd / lax.optimization_barrier(jnp.sum(expd, axis=-1, keepdims=True))).astype(jnp.bfloat16)
    return jnp.dot(probs, value_rows, preferred_element_type=jnp.float32).astype(jnp.bfloat16)

def reference(resid, queries, keys, values, forget_cache, query_gain, key_gain, out_weight, norm_gain, routes, group_weight, inner_share, expert_gate, expert_up, expert_down):

    def sequence_attention(operands):
        seq_q, seq_k, seq_v, seq_c = operands
        query_normed = norm_rows(seq_q.reshape(SEQUENCE_LENGTH, HEAD_COUNT, HD), query_gain).transpose(1, 0, 2)
        key_normed = norm_rows(seq_k.reshape(SEQUENCE_LENGTH, HEAD_COUNT, HD), key_gain).transpose(1, 0, 2)
        value_heads = seq_v.reshape(SEQUENCE_LENGTH, HEAD_COUNT, HD).transpose(1, 0, 2)
        outputs = lax.map(head_attention, (query_normed, key_normed, value_heads, seq_c))
        return outputs.transpose(1, 0, 2).reshape(SEQUENCE_LENGTH, HEAD_COUNT * HD)
    attn = lax.map(sequence_attention, (queries, keys, values, forget_cache))
    projected = jnp.dot(attn.reshape(-1, HEAD_COUNT * HD), out_weight, preferred_element_type=jnp.float32)
    mid = (resid.reshape(-1, D).astype(jnp.float32) + projected).astype(jnp.bfloat16)
    normed = norm_rows(mid, norm_gain)
    shares = inner_share.reshape(-1, TOPK).astype(jnp.float32)
    weights = group_weight.reshape(-1, 1).astype(jnp.float32) * shares / lax.optimization_barrier(jnp.sum(shares, axis=-1, keepdims=True))
    flat_weights = weights.reshape(-1)
    flat_routes = routes.reshape(-1).astype(jnp.int32)
    slot_count = EXPERTS * CAP
    slot_place = jnp.arange(slot_count, dtype=jnp.int32)

    def one_expert(total, expert_index):
        hit = flat_routes == expert_index
        hit_count = jnp.sum(hit.astype(jnp.int32))
        picked = jnp.nonzero(hit, size=slot_count, fill_value=0)[0].astype(jnp.int32)
        live = slot_place < hit_count
        token_index = (picked // TOPK).astype(jnp.int32)
        rows = normed[token_index]
        gate = jnp.dot(rows, expert_gate[expert_index], preferred_element_type=jnp.float32)
        upper = jnp.dot(rows, expert_up[expert_index], preferred_element_type=jnp.float32)
        hidden = (jax.nn.silu(gate) * upper).astype(jnp.bfloat16)
        result = jnp.dot(hidden, expert_down[expert_index], preferred_element_type=jnp.float32).astype(jnp.bfloat16)
        scale = jnp.where(live, flat_weights[picked], jnp.zeros_like(flat_weights[picked]))
        total = total.at[token_index].add(result.astype(jnp.float32) * scale[:, None])
        return (total, None)
    start = jnp.zeros((mid.shape[0], D), jnp.float32)
    mixed, _ = lax.scan(one_expert, start, jnp.arange(EXPERTS, dtype=jnp.int32))
    layer_out = (mid.astype(jnp.float32) + mixed).astype(jnp.bfloat16)
    return layer_out.reshape(SEQUENCE_COUNT, SEQUENCE_LENGTH, D)
```

```python
import functools

import jax
import jax.numpy as jnp
from jax import lax
from jax.experimental import pallas as pl
from jax.experimental.pallas import tpu as pltpu
from jax.sharding import PartitionSpec as P

EPS = 1e-06


def norm_rows(inputs, gain):
    floats = inputs.astype(jnp.float32)
    scaled = floats * lax.rsqrt(jnp.mean(floats * floats, axis=-1, keepdims=True) + EPS)
    return (scaled * gain).astype(jnp.bfloat16)


LANES = 128
ROWS = 256


def pack_kernel(query_ref, key_ref, value_ref, *out_refs):
    lanes = out_refs[0].shape[2]
    tokens = query_ref.shape[0]
    chunks = len(out_refs)
    for peer in range(out_refs[0].shape[0]):
        for chunk in range(chunks):
            start = (peer * chunks + chunk) * lanes
            for place, ref in enumerate((query_ref, key_ref, value_ref)):
                out_refs[chunk][peer, place * tokens : (place + 1) * tokens, :] = ref[
                    :, start : start + lanes
                ]


def pack_heads(queries, keys, values, peers, chunks, lanes):
    tokens = queries.shape[0]
    shape = jax.ShapeDtypeStruct((peers, 3 * tokens, lanes), queries.dtype)
    return pl.pallas_call(
        pack_kernel,
        out_shape=[shape] * chunks,
        name="pack_heads",
        cost_estimate=pl.CostEstimate(
            flops=queries.size, bytes_accessed=12 * queries.size, transcendentals=0
        ),
    )(queries, keys, values)


def attend_kernel(
    tokens, head_size, rows, qkv_ref, gains_ref, level_ref, column_ref, out_ref, q_ref, k_ref, v_ref
):
    peers, _, lanes = qkv_ref.shape
    length = peers * tokens
    packed = lanes // head_size
    scale = head_size ** (-0.5)
    lane_head = lax.broadcasted_iota(jnp.int32, (1, lanes), 1) // head_size
    same = (
        lax.broadcasted_iota(jnp.int32, (lanes, lanes), 0) // head_size
        == lax.broadcasted_iota(jnp.int32, (lanes, lanes), 1) // head_size
    ).astype(jnp.bfloat16)

    def normed(part, gain):
        floats = part.astype(jnp.float32)
        squares = floats * floats
        high = squares.astype(jnp.bfloat16)
        low = (squares - high.astype(jnp.float32)).astype(jnp.bfloat16)
        total = jnp.dot(high, same, preferred_element_type=jnp.float32) + jnp.dot(
            low, same, preferred_element_type=jnp.float32
        )
        return (floats * lax.rsqrt(total * (1.0 / head_size) + EPS) * gain).astype(jnp.bfloat16)

    for peer in range(peers):
        place = slice(peer * tokens, (peer + 1) * tokens)
        query = normed(qkv_ref[peer, :tokens, :], gains_ref[0:1, :])
        key = normed(qkv_ref[peer, tokens : 2 * tokens, :], gains_ref[1:2, :])
        value = qkv_ref[peer, 2 * tokens :, :]
        k_ref[place, :] = key
        for head in range(packed):
            own = lane_head == head
            q_ref[head, place, :] = jnp.where(own, query, jnp.zeros_like(query))
            v_ref[head, place, :] = jnp.where(own, value, jnp.ones_like(value))

    inside = lax.broadcasted_iota(jnp.int32, (rows, rows), 1) <= lax.broadcasted_iota(
        jnp.int32, (rows, rows), 0
    )
    contract = (((1,), (1,)), ((), ()))
    for start in range(0, length, rows):
        stop = start + rows
        outs = []
        for head in range(packed):
            query = q_ref[head, start:stop, :]
            row_level = column_ref[start:stop, head : head + 1]
            last = lax.dot_general(
                query, k_ref[start:stop, :], contract, preferred_element_type=jnp.float32
            )
            last = jnp.where(inside, last * scale - level_ref[head : head + 1, start:stop], -jnp.inf)
            highest = jnp.max(last, axis=1, keepdims=True)
            if start:
                early = lax.dot_general(
                    query, k_ref[:start, :], contract, preferred_element_type=jnp.float32
                )
                early = early * scale - level_ref[head : head + 1, :start]
                highest = jnp.maximum(highest, jnp.max(early, axis=1, keepdims=True))
            shift = row_level - (highest + row_level)
            out = jnp.dot(
                jnp.exp(last + shift).astype(jnp.bfloat16),
                v_ref[head, start:stop, :],
                preferred_element_type=jnp.float32,
            )
            if start:
                out = out + jnp.dot(
                    jnp.exp(early + shift).astype(jnp.bfloat16),
                    v_ref[head, :start, :],
                    preferred_element_type=jnp.float32,
                )
            outs.append(out)
        numerator, sums = outs[0], outs[1]
        for head in range(1, packed):
            numerator = jnp.where(lane_head == head, outs[head], numerator)
            sums = jnp.where(lane_head == head, outs[head - 1], sums)
        sums = pltpu.roll(sums, head_size, 1) if packed == 2 else sum_lanes(outs, lane_head, head_size)
        out_ref[start:stop, :] = (numerator / sums).astype(out_ref.dtype)


def sum_lanes(outs, lane_head, head_size):
    packed = len(outs)
    total = jnp.zeros_like(outs[0])
    for head in range(packed):
        other = (head + 1) % packed * head_size
        total = jnp.where(lane_head == head, outs[head][:, other : other + 1], total)
    return total


def attend(qkv, gains, level, level_columns, tokens, head_size):
    peers, _, lanes = qkv.shape
    length = peers * tokens
    packed = lanes // head_size
    rows = ROWS if length % ROWS == 0 else tokens
    return pl.pallas_call(
        functools.partial(attend_kernel, tokens, head_size, rows),
        out_shape=jax.ShapeDtypeStruct((length, lanes), jnp.bfloat16),
        scratch_shapes=[
            pltpu.VMEM((packed, length, lanes), jnp.bfloat16),
            pltpu.VMEM((length, lanes), jnp.bfloat16),
            pltpu.VMEM((packed, length, lanes), jnp.bfloat16),
        ],
        compiler_params=pltpu.CompilerParams(vmem_limit_bytes=32 * 1024 * 1024),
        name="attend",
        cost_estimate=pl.CostEstimate(
            flops=4 * packed * length * length * lanes,
            bytes_accessed=8 * length * lanes,
            transcendentals=packed * length * length,
        ),
    )(qkv, gains, level, level_columns)


def gather_shards(shard, axis):
    size = lax.axis_size(axis)
    held = [shard]
    stride = size // 2
    offsets = [0]
    while stride:
        pairs = [(index, index ^ stride) for index in range(size)]
        held = held + [lax.ppermute(part, axis, pairs) for part in held]
        offsets = offsets + [offset ^ stride for offset in offsets]
        stride //= 2
    ordered = [None] * size
    for part, offset in zip(held, offsets):
        ordered[offset] = part
    return ordered


def order_pieces(pieces, axis):
    size = lax.axis_size(axis)
    own = lax.axis_index(axis)
    stride = 1
    while stride < size:
        flip = (own & stride) != 0
        pieces = [
            jnp.where(flip, pieces[index ^ stride], pieces[index]) for index in range(size)
        ]
        stride *= 2
    return pieces


def shards(
    resid,
    queries,
    keys,
    values,
    forget_cache,
    query_gain,
    key_gain,
    out_weight,
    norm_gain,
    routes,
    group_weight,
    inner_share,
    expert_gate,
    expert_up,
    expert_down,
):
    dp_size = lax.axis_size("dp")
    sp_size = lax.axis_size("sp")
    tokens = queries.shape[1]
    head_size = query_gain.shape[0]
    local_heads = forget_cache.shape[1]
    local_width = local_heads * head_size
    lanes = LANES if local_width % LANES == 0 else local_width
    chunks = local_width // lanes
    packed = lanes // head_size
    sends = pack_heads(queries[0], keys[0], values[0], sp_size, chunks, lanes)
    arrived_qkv = [
        lax.all_to_all(send, "sp", split_axis=0, concat_axis=0, tiled=True) for send in sends
    ]
    weight_shards = gather_shards(out_weight, "dp")
    gains = jnp.stack([jnp.tile(query_gain, packed), jnp.tile(key_gain, packed)])
    level = forget_cache[0]
    level_columns = level.T
    returned_heads = []
    for chunk in range(chunks):
        first = chunk * packed
        block = attend(
            arrived_qkv[chunk],
            gains,
            level[first : first + packed],
            level_columns[:, first : first + packed],
            tokens,
            head_size,
        )
        returned_heads.append(
            lax.all_to_all(
                block.reshape(sp_size, tokens, lanes),
                "sp",
                split_axis=0,
                concat_axis=0,
                tiled=True,
            )
        )
    token_attn = (
        jnp.stack(returned_heads, axis=1)
        .transpose(2, 0, 1, 3)
        .reshape(tokens, sp_size * local_width)
    )
    pieces = [
        jnp.dot(token_attn, shard, preferred_element_type=jnp.float32) for shard in weight_shards
    ]
    pieces = order_pieces(pieces, "dp")
    projected = jnp.concatenate(pieces, axis=1)
    mid = (resid[0].astype(jnp.float32) + projected).astype(jnp.bfloat16)
    normed = norm_rows(mid, norm_gain)
    width = normed.shape[1]
    tok_count = normed.shape[0]
    top_count = routes.shape[2]
    experts = lax.axis_size("sp") * lax.axis_size("dp")
    capacity = 2 * tok_count * top_count // experts
    expert_ids = routes[0].reshape(-1)
    expert_onehot = (expert_ids[:, None] == jnp.arange(experts, dtype=jnp.int32)[None, :]).astype(
        jnp.int32
    )
    earlier = jnp.cumsum(expert_onehot, axis=0) - expert_onehot
    slot_rank = jnp.sum(earlier * expert_onehot, axis=1)
    slot_index = (expert_ids * capacity + slot_rank).reshape(tok_count, top_count)
    slot_range = jnp.arange(experts * capacity, dtype=jnp.int32)
    dispatch = jnp.any(slot_range[:, None, None] == slot_index[None, :, :], axis=2).astype(
        jnp.bfloat16
    )
    send = jnp.dot(dispatch, normed, preferred_element_type=jnp.float32).astype(jnp.bfloat16)
    arrived = lax.all_to_all(
        send.reshape(experts, capacity, width),
        ("sp", "dp"),
        split_axis=0,
        concat_axis=0,
        tiled=True,
    )
    flat_rows = arrived.reshape(-1, width)
    gate = jnp.dot(flat_rows, expert_gate[0], preferred_element_type=jnp.float32)
    upper = jnp.dot(flat_rows, expert_up[0], preferred_element_type=jnp.float32)
    hidden = (jax.nn.silu(gate) * upper).astype(jnp.bfloat16)
    result = jnp.dot(hidden, expert_down[0], preferred_element_type=jnp.float32).astype(
        jnp.bfloat16
    )
    returned = lax.all_to_all(
        result.reshape(arrived.shape), ("sp", "dp"), split_axis=0, concat_axis=0, tiled=True
    )
    returned = returned.reshape(experts * capacity, width)
    shares = inner_share[0]
    weights = group_weight[0][:, None] * shares / jnp.sum(shares, axis=-1, keepdims=True)
    mixed = jnp.zeros((tok_count, width), jnp.float32)
    for route in range(top_count):
        select = (slot_range[None, :] == slot_index[:, route : route + 1]).astype(jnp.bfloat16)
        picked = jnp.dot(select, returned, preferred_element_type=jnp.float32)
        mixed = mixed + weights[:, route : route + 1] * picked
    layer_out = (mid.astype(jnp.float32) + mixed).astype(jnp.bfloat16)
    return layer_out.reshape(1, tok_count, width)


def solution(mesh):
    return jax.shard_map(
        shards,
        mesh=mesh,
        in_specs=(
            P("dp", "sp", None),
            P("dp", "sp", None),
            P("dp", "sp", None),
            P("dp", "sp", None),
            P("dp", "sp", None),
            P(),
            P(),
            P(None, "dp"),
            P(),
            P("dp", "sp", None),
            P("dp", "sp"),
            P("dp", "sp", None),
            P(("sp", "dp"), None, None),
            P(("sp", "dp"), None, None),
            P(("sp", "dp"), None, None),
        ),
        out_specs=P("dp", "sp", None),
        check_vma=False,
    )
```

```python
import functools

import jax
import jax.numpy as jnp
from jax import lax
from jax.experimental import pallas as pl
from jax.experimental.pallas import tpu as pltpu
from jax.sharding import PartitionSpec as P

EPS = 1e-06


def norm_rows(inputs, gain):
    floats = inputs.astype(jnp.float32)
    scaled = floats * lax.rsqrt(jnp.mean(floats * floats, axis=-1, keepdims=True) + EPS)
    return (scaled * gain).astype(jnp.bfloat16)


LANES = 128
SEQ = ("hi", "lo")
ROWS = 256


def pack_kernel(query_ref, key_ref, value_ref, *out_refs):
    lanes = out_refs[0].shape[2]
    tokens = query_ref.shape[0]
    chunks = len(out_refs)
    for peer in range(out_refs[0].shape[0]):
        for chunk in range(chunks):
            start = (peer * chunks + chunk) * lanes
            for place, ref in enumerate((query_ref, key_ref, value_ref)):
                out_refs[chunk][peer, place * tokens : (place + 1) * tokens, :] = ref[
                    :, start : start + lanes
                ]


def pack_heads(queries, keys, values, peers, chunks, lanes):
    tokens = queries.shape[0]
    shape = jax.ShapeDtypeStruct((peers, 3 * tokens, lanes), queries.dtype)
    return pl.pallas_call(
        pack_kernel,
        out_shape=[shape] * chunks,
        name="pack_heads",
        cost_estimate=pl.CostEstimate(
            flops=queries.size, bytes_accessed=12 * queries.size, transcendentals=0
        ),
    )(queries, keys, values)


def attend_kernel(
    tokens, head_size, rows, qkv_ref, gains_ref, level_ref, column_ref, out_ref, q_ref, k_ref, v_ref
):
    peers, _, lanes = qkv_ref.shape
    length = peers * tokens
    packed = lanes // head_size
    scale = head_size ** (-0.5)
    lane_head = lax.broadcasted_iota(jnp.int32, (1, lanes), 1) // head_size
    same = (
        lax.broadcasted_iota(jnp.int32, (lanes, lanes), 0) // head_size
        == lax.broadcasted_iota(jnp.int32, (lanes, lanes), 1) // head_size
    ).astype(jnp.bfloat16)

    def normed(part, gain):
        floats = part.astype(jnp.float32)
        squares = floats * floats
        high = squares.astype(jnp.bfloat16)
        low = (squares - high.astype(jnp.float32)).astype(jnp.bfloat16)
        total = jnp.dot(high, same, preferred_element_type=jnp.float32) + jnp.dot(
            low, same, preferred_element_type=jnp.float32
        )
        return (floats * lax.rsqrt(total * (1.0 / head_size) + EPS) * gain).astype(jnp.bfloat16)

    for peer in range(peers):
        place = slice(peer * tokens, (peer + 1) * tokens)
        query = normed(qkv_ref[peer, :tokens, :], gains_ref[0:1, :])
        key = normed(qkv_ref[peer, tokens : 2 * tokens, :], gains_ref[1:2, :])
        value = qkv_ref[peer, 2 * tokens :, :]
        k_ref[place, :] = key
        for head in range(packed):
            own = lane_head == head
            q_ref[head, place, :] = jnp.where(own, query, jnp.zeros_like(query))
            v_ref[head, place, :] = jnp.where(own, value, jnp.ones_like(value))

    inside = lax.broadcasted_iota(jnp.int32, (rows, rows), 1) <= lax.broadcasted_iota(
        jnp.int32, (rows, rows), 0
    )
    contract = (((1,), (1,)), ((), ()))
    for start in range(0, length, rows):
        stop = start + rows
        outs = []
        for head in range(packed):
            query = q_ref[head, start:stop, :]
            row_level = column_ref[start:stop, head : head + 1]
            last = lax.dot_general(
                query, k_ref[start:stop, :], contract, preferred_element_type=jnp.float32
            )
            last = jnp.where(inside, last * scale - level_ref[head : head + 1, start:stop], -jnp.inf)
            highest = jnp.max(last, axis=1, keepdims=True)
            if start:
                early = lax.dot_general(
                    query, k_ref[:start, :], contract, preferred_element_type=jnp.float32
                )
                early = early * scale - level_ref[head : head + 1, :start]
                highest = jnp.maximum(highest, jnp.max(early, axis=1, keepdims=True))
            shift = row_level - (highest + row_level)
            out = jnp.dot(
                jnp.exp(last + shift).astype(jnp.bfloat16),
                v_ref[head, start:stop, :],
                preferred_element_type=jnp.float32,
            )
            if start:
                out = out + jnp.dot(
                    jnp.exp(early + shift).astype(jnp.bfloat16),
                    v_ref[head, :start, :],
                    preferred_element_type=jnp.float32,
                )
            outs.append(out)
        numerator, sums = outs[0], outs[1]
        for head in range(1, packed):
            numerator = jnp.where(lane_head == head, outs[head], numerator)
            sums = jnp.where(lane_head == head, outs[head - 1], sums)
        sums = pltpu.roll(sums, head_size, 1) if packed == 2 else sum_lanes(outs, lane_head, head_size)
        out_ref[start:stop, :] = (numerator / sums).astype(out_ref.dtype)


def sum_lanes(outs, lane_head, head_size):
    packed = len(outs)
    total = jnp.zeros_like(outs[0])
    for head in range(packed):
        other = (head + 1) % packed * head_size
        total = jnp.where(lane_head == head, outs[head][:, other : other + 1], total)
    return total


def attend(qkv, gains, level, level_columns, tokens, head_size):
    peers, _, lanes = qkv.shape
    length = peers * tokens
    packed = lanes // head_size
    rows = ROWS if length % ROWS == 0 else tokens
    return pl.pallas_call(
        functools.partial(attend_kernel, tokens, head_size, rows),
        out_shape=jax.ShapeDtypeStruct((length, lanes), jnp.bfloat16),
        scratch_shapes=[
            pltpu.VMEM((packed, length, lanes), jnp.bfloat16),
            pltpu.VMEM((length, lanes), jnp.bfloat16),
            pltpu.VMEM((packed, length, lanes), jnp.bfloat16),
        ],
        compiler_params=pltpu.CompilerParams(vmem_limit_bytes=32 * 1024 * 1024),
        name="attend",
        cost_estimate=pl.CostEstimate(
            flops=4 * packed * length * length * lanes,
            bytes_accessed=8 * length * lanes,
            transcendentals=packed * length * length,
        ),
    )(qkv, gains, level, level_columns)


def tie_kernel(*refs):
    del refs


def tie(part, *after):
    anywhere = pl.BlockSpec(memory_space=pl.ANY)
    after = [array.reshape(-1, array.shape[-1])[:8, :LANES] for array in after]
    return pl.pallas_call(
        tie_kernel,
        out_shape=jax.ShapeDtypeStruct(part.shape, part.dtype),
        in_specs=[anywhere] * (1 + len(after)),
        out_specs=anywhere,
        input_output_aliases={0: 0},
        name="tie",
    )(part, *after)


def xor_pairs(size, stride):
    return [(index, index ^ stride) for index in range(size)]


def gather_start(shard, axis):
    size = lax.axis_size(axis)
    return [shard, lax.ppermute(shard, axis, xor_pairs(size, size // 2))]


def gather_rest(held, axis, after):
    size = lax.axis_size(axis)
    held = [held[0], tie(held[1], *after)]
    offsets = [0, size // 2]
    stride = size // 4
    while stride:
        held = held + [lax.ppermute(part, axis, xor_pairs(size, stride)) for part in held]
        offsets = offsets + [offset ^ stride for offset in offsets]
        stride //= 2
    ordered = [None] * size
    for part, offset in zip(held, offsets):
        ordered[offset] = part
    return ordered


def order_pieces(pieces, axis):
    size = lax.axis_size(axis)
    own = lax.axis_index(axis)
    stride = 1
    while stride < size:
        flip = (own & stride) != 0
        pieces = [
            jnp.where(flip, pieces[index ^ stride], pieces[index]) for index in range(size)
        ]
        stride *= 2
    return pieces


def shards(
    resid,
    queries,
    keys,
    values,
    forget_cache,
    query_gain,
    key_gain,
    out_weight,
    norm_gain,
    routes,
    group_weight,
    inner_share,
    expert_gate,
    expert_up,
    expert_down,
):
    dp_size = lax.axis_size("dp")
    sp_size = lax.axis_size("hi") * lax.axis_size("lo")
    tokens = queries.shape[1]
    head_size = query_gain.shape[0]
    local_heads = forget_cache.shape[1]
    local_width = local_heads * head_size
    lanes = LANES if local_width % LANES == 0 else local_width
    chunks = local_width // lanes
    packed = lanes // head_size
    sends = pack_heads(queries[0], keys[0], values[0], sp_size, chunks, lanes)
    arrived_qkv = [
        lax.all_to_all(send, SEQ, split_axis=0, concat_axis=0, tiled=True) for send in sends
    ]
    weight_shards = gather_start(out_weight, "dp")
    gains = jnp.stack([jnp.tile(query_gain, packed), jnp.tile(key_gain, packed)])
    level = forget_cache[0]
    level_columns = level.T
    returned_heads = []
    blocks = []
    for chunk in range(chunks):
        first = chunk * packed
        block = attend(
            arrived_qkv[chunk],
            gains,
            level[first : first + packed],
            level_columns[:, first : first + packed],
            tokens,
            head_size,
        )
        blocks.append(block)
        returned_heads.append(
            lax.all_to_all(
                block.reshape(sp_size, tokens, lanes),
                SEQ,
                split_axis=0,
                concat_axis=0,
                tiled=True,
            )
        )
    weight_shards = gather_rest(weight_shards, "dp", blocks)
    token_attn = (
        jnp.stack(returned_heads, axis=1)
        .transpose(2, 0, 1, 3)
        .reshape(tokens, sp_size * local_width)
    )
    pieces = [
        jnp.dot(token_attn, shard, preferred_element_type=jnp.float32) for shard in weight_shards
    ]
    pieces = order_pieces(pieces, "dp")
    projected = jnp.concatenate(pieces, axis=1)
    mid = (resid[0].astype(jnp.float32) + projected).astype(jnp.bfloat16)
    normed = norm_rows(mid, norm_gain)
    width = normed.shape[1]
    top_count = routes.shape[2]
    swap = [(0, 1), (1, 0)]
    half = sp_size * dp_size // 2
    capacity = tokens * top_count // half
    shares = inner_share[0]
    weights = group_weight[0][:, None] * shares / jnp.sum(shares, axis=-1, keepdims=True)
    own_slots = slots_of(routes[0], half, capacity)
    far_slots = slots_of(lax.ppermute(routes[0], "hi", swap), half, capacity)
    far_weights = lax.ppermute(weights, "hi", swap)
    far_normed = lax.ppermute(normed, "hi", swap)
    experts = (expert_gate[0], expert_up[0], expert_down[0])
    own_rows = exchange(spread(normed, own_slots, half, capacity))
    far_normed = tie(far_normed, own_rows)
    far_rows = exchange(spread(far_normed, far_slots, half, capacity))
    own_result = expert_of(own_rows, *experts)
    far_back = exchange(expert_of(far_rows, *experts))
    own_back = exchange(tie(own_result, far_back))
    far_mixed = gather_back(far_back, far_slots, far_weights).astype(jnp.bfloat16)
    other = lax.ppermute(far_mixed, "hi", swap)
    mixed = gather_back(own_back, own_slots, weights) + other.astype(jnp.float32)
    layer_out = (mid.astype(jnp.float32) + mixed).astype(jnp.bfloat16)
    return layer_out.reshape(1, tokens, width)


def slots_of(ids, half, capacity):
    tok_count, top_count = ids.shape
    flat = ids.reshape(-1)
    onehot = (flat[:, None] == jnp.arange(2 * half, dtype=jnp.int32)[None, :]).astype(jnp.int32)
    earlier = jnp.cumsum(onehot, axis=0) - onehot
    rank = jnp.sum(earlier * onehot, axis=1)
    return ((flat - lax.axis_index("hi") * half) * capacity + rank).reshape(tok_count, top_count)


def spread(rows, slots, half, capacity):
    slot_range = jnp.arange(half * capacity, dtype=jnp.int32)
    dispatch = jnp.any(slot_range[:, None, None] == slots[None, :, :], axis=2)
    send = jnp.dot(dispatch.astype(jnp.bfloat16), rows, preferred_element_type=jnp.float32)
    return send.astype(jnp.bfloat16).reshape(half, capacity, rows.shape[1])


def exchange(rows):
    return lax.all_to_all(rows, ("lo", "dp"), split_axis=0, concat_axis=0, tiled=True)


def expert_of(rows, gate_weight, up_weight, down_weight):
    flat = rows.reshape(-1, rows.shape[2])
    gate = jnp.dot(flat, gate_weight, preferred_element_type=jnp.float32)
    upper = jnp.dot(flat, up_weight, preferred_element_type=jnp.float32)
    hidden = (jax.nn.silu(gate) * upper).astype(jnp.bfloat16)
    result = jnp.dot(hidden, down_weight, preferred_element_type=jnp.float32)
    return result.astype(jnp.bfloat16).reshape(rows.shape)


def gather_back(returned, slots, weights):
    flat = returned.reshape(-1, returned.shape[2])
    slot_range = jnp.arange(flat.shape[0], dtype=jnp.int32)
    mixed = jnp.zeros((slots.shape[0], flat.shape[1]), jnp.float32)
    for route in range(slots.shape[1]):
        select = (slot_range[None, :] == slots[:, route : route + 1]).astype(jnp.bfloat16)
        picked = jnp.dot(select, flat, preferred_element_type=jnp.float32)
        mixed = mixed + weights[:, route : route + 1] * picked
    return mixed


def solution(mesh):
    sizes = mesh.shape
    mesh = jax.sharding.Mesh(
        mesh.devices.reshape(2, sizes["sp"] // 2, sizes["dp"]), ("hi", "lo", "dp")
    )
    return jax.shard_map(
        shards,
        mesh=mesh,
        in_specs=(
            P("dp", SEQ, None),
            P("dp", SEQ, None),
            P("dp", SEQ, None),
            P("dp", SEQ, None),
            P("dp", SEQ, None),
            P(),
            P(),
            P(None, "dp"),
            P(),
            P("dp", SEQ, None),
            P("dp", SEQ),
            P("dp", SEQ, None),
            P(("hi", "lo", "dp"), None, None),
            P(("hi", "lo", "dp"), None, None),
            P(("hi", "lo", "dp"), None, None),
        ),
        out_specs=P("dp", SEQ, None),
        check_vma=False,
    )
```

```python
import functools

import jax
import jax.numpy as jnp
from jax import lax
from jax.experimental import pallas as pl
from jax.experimental.pallas import tpu as pltpu
from jax.sharding import PartitionSpec as P

EPS = 1e-06


def norm_rows(inputs, gain):
    floats = inputs.astype(jnp.float32)
    scaled = floats * lax.rsqrt(jnp.mean(floats * floats, axis=-1, keepdims=True) + EPS)
    return (scaled * gain).astype(jnp.bfloat16)


LANES = 128
SEQ = "sp"
ROWS = 256
UNITS = 256


def pack_kernel(query_ref, key_ref, value_ref, *out_refs):
    lanes = out_refs[0].shape[2]
    tokens = query_ref.shape[0]
    chunks = len(out_refs)
    for peer in range(out_refs[0].shape[0]):
        for chunk in range(chunks):
            start = (peer * chunks + chunk) * lanes
            for place, ref in enumerate((query_ref, key_ref, value_ref)):
                out_refs[chunk][peer, place * tokens : (place + 1) * tokens, :] = ref[
                    :, start : start + lanes
                ]


def pack_heads(queries, keys, values, peers, chunks, lanes):
    tokens = queries.shape[0]
    shape = jax.ShapeDtypeStruct((peers, 3 * tokens, lanes), queries.dtype)
    return pl.pallas_call(
        pack_kernel,
        out_shape=[shape] * chunks,
        name="pack_heads",
        cost_estimate=pl.CostEstimate(
            flops=queries.size, bytes_accessed=12 * queries.size, transcendentals=0
        ),
    )(queries, keys, values)


def attend_kernel(
    tokens, head_size, rows, qkv_ref, gains_ref, level_ref, column_ref, out_ref, q_ref, k_ref, v_ref
):
    peers, _, lanes = qkv_ref.shape
    length = peers * tokens
    packed = lanes // head_size
    scale = head_size ** (-0.5)
    lane_head = lax.broadcasted_iota(jnp.int32, (1, lanes), 1) // head_size
    same = (
        lax.broadcasted_iota(jnp.int32, (lanes, lanes), 0) // head_size
        == lax.broadcasted_iota(jnp.int32, (lanes, lanes), 1) // head_size
    ).astype(jnp.bfloat16)

    def normed(part, gain):
        floats = part.astype(jnp.float32)
        squares = floats * floats
        high = squares.astype(jnp.bfloat16)
        low = (squares - high.astype(jnp.float32)).astype(jnp.bfloat16)
        total = jnp.dot(high, same, preferred_element_type=jnp.float32) + jnp.dot(
            low, same, preferred_element_type=jnp.float32
        )
        return (floats * lax.rsqrt(total * (1.0 / head_size) + EPS) * gain).astype(jnp.bfloat16)

    for peer in range(peers):
        place = slice(peer * tokens, (peer + 1) * tokens)
        query = normed(qkv_ref[peer, :tokens, :], gains_ref[0:1, :])
        key = normed(qkv_ref[peer, tokens : 2 * tokens, :], gains_ref[1:2, :])
        value = qkv_ref[peer, 2 * tokens :, :]
        k_ref[place, :] = key
        for head in range(packed):
            own = lane_head == head
            q_ref[head, place, :] = jnp.where(own, query, jnp.zeros_like(query))
            v_ref[head, place, :] = jnp.where(own, value, jnp.ones_like(value))

    inside = lax.broadcasted_iota(jnp.int32, (rows, rows), 1) <= lax.broadcasted_iota(
        jnp.int32, (rows, rows), 0
    )
    contract = (((1,), (1,)), ((), ()))
    for start in range(0, length, rows):
        stop = start + rows
        outs = []
        for head in range(packed):
            query = q_ref[head, start:stop, :]
            row_level = column_ref[start:stop, head : head + 1]
            last = lax.dot_general(
                query, k_ref[start:stop, :], contract, preferred_element_type=jnp.float32
            )
            last = jnp.where(inside, last * scale - level_ref[head : head + 1, start:stop], -jnp.inf)
            highest = jnp.max(last, axis=1, keepdims=True)
            if start:
                early = lax.dot_general(
                    query, k_ref[:start, :], contract, preferred_element_type=jnp.float32
                )
                early = early * scale - level_ref[head : head + 1, :start]
                highest = jnp.maximum(highest, jnp.max(early, axis=1, keepdims=True))
            shift = row_level - (highest + row_level)
            out = jnp.dot(
                jnp.exp(last + shift).astype(jnp.bfloat16),
                v_ref[head, start:stop, :],
                preferred_element_type=jnp.float32,
            )
            if start:
                out = out + jnp.dot(
                    jnp.exp(early + shift).astype(jnp.bfloat16),
                    v_ref[head, :start, :],
                    preferred_element_type=jnp.float32,
                )
            outs.append(out)
        numerator, sums = outs[0], outs[1]
        for head in range(1, packed):
            numerator = jnp.where(lane_head == head, outs[head], numerator)
            sums = jnp.where(lane_head == head, outs[head - 1], sums)
        sums = pltpu.roll(sums, head_size, 1) if packed == 2 else sum_lanes(outs, lane_head, head_size)
        out_ref[start:stop, :] = (numerator / sums).astype(out_ref.dtype)


def sum_lanes(outs, lane_head, head_size):
    packed = len(outs)
    total = jnp.zeros_like(outs[0])
    for head in range(packed):
        other = (head + 1) % packed * head_size
        total = jnp.where(lane_head == head, outs[head][:, other : other + 1], total)
    return total


def attend(qkv, gains, level, level_columns, tokens, head_size):
    peers, _, lanes = qkv.shape
    length = peers * tokens
    packed = lanes // head_size
    rows = ROWS if length % ROWS == 0 else tokens
    return pl.pallas_call(
        functools.partial(attend_kernel, tokens, head_size, rows),
        out_shape=jax.ShapeDtypeStruct((length, lanes), jnp.bfloat16),
        scratch_shapes=[
            pltpu.VMEM((packed, length, lanes), jnp.bfloat16),
            pltpu.VMEM((length, lanes), jnp.bfloat16),
            pltpu.VMEM((packed, length, lanes), jnp.bfloat16),
        ],
        compiler_params=pltpu.CompilerParams(vmem_limit_bytes=32 * 1024 * 1024),
        name="attend",
        cost_estimate=pl.CostEstimate(
            flops=4 * packed * length * length * lanes,
            bytes_accessed=8 * length * lanes,
            transcendentals=packed * length * length,
        ),
    )(qkv, gains, level, level_columns)


def tie_kernel(*refs):
    del refs


def tie(part, *after):
    anywhere = pl.BlockSpec(memory_space=pl.ANY)
    after = [array.reshape(-1, array.shape[-1])[:8, :LANES] for array in after]
    return pl.pallas_call(
        tie_kernel,
        out_shape=jax.ShapeDtypeStruct(part.shape, part.dtype),
        in_specs=[anywhere] * (1 + len(after)),
        out_specs=anywhere,
        input_output_aliases={0: 0},
        name="tie",
    )(part, *after)


def xor_pairs(size, stride):
    return [(index, index ^ stride) for index in range(size)]


def gather_start(shard, axis):
    size = lax.axis_size(axis)
    return [shard, lax.ppermute(shard, axis, xor_pairs(size, size // 2))]


def gather_rest(held, axis, after):
    size = lax.axis_size(axis)
    held = [held[0], tie(held[1], *after)]
    offsets = [0, size // 2]
    stride = size // 4
    while stride:
        held = held + [lax.ppermute(part, axis, xor_pairs(size, stride)) for part in held]
        offsets = offsets + [offset ^ stride for offset in offsets]
        stride //= 2
    ordered = [None] * size
    for part, offset in zip(held, offsets):
        ordered[offset] = part
    return ordered


def order_pieces(pieces, axis):
    size = lax.axis_size(axis)
    own = lax.axis_index(axis)
    stride = 1
    while stride < size:
        flip = (own & stride) != 0
        pieces = [
            jnp.where(flip, pieces[index ^ stride], pieces[index]) for index in range(size)
        ]
        stride *= 2
    return pieces


def expert_kernel(rows_ref, gate_ref, up_ref, down_ref, out_ref, total_ref):
    step = pl.program_id(0)
    rows = rows_ref[...]
    gate = jnp.dot(rows, gate_ref[...], preferred_element_type=jnp.float32)
    upper = jnp.dot(rows, up_ref[...], preferred_element_type=jnp.float32)
    hidden = (gate / (1.0 + jnp.exp(-gate)) * upper).astype(jnp.bfloat16)
    part = jnp.dot(hidden, down_ref[...], preferred_element_type=jnp.float32)

    @pl.when(step == 0)
    def _():
        total_ref[...] = part

    @pl.when(step > 0)
    def _():
        total_ref[...] += part

    @pl.when(step == pl.num_programs(0) - 1)
    def _():
        out_ref[...] = total_ref[...].astype(out_ref.dtype)


def expert_of(rows, gate_weight, up_weight, down_weight):
    count, width = rows.shape
    units = gate_weight.shape[1]
    tile = UNITS if units % UNITS == 0 else units
    return pl.pallas_call(
        expert_kernel,
        grid=(units // tile,),
        out_shape=jax.ShapeDtypeStruct((count, width), jnp.bfloat16),
        in_specs=[
            pl.BlockSpec((count, width), lambda step: (0, 0)),
            pl.BlockSpec((width, tile), lambda step: (0, step)),
            pl.BlockSpec((width, tile), lambda step: (0, step)),
            pl.BlockSpec((tile, width), lambda step: (step, 0)),
        ],
        out_specs=pl.BlockSpec((count, width), lambda step: (0, 0)),
        scratch_shapes=[pltpu.VMEM((count, width), jnp.float32)],
        compiler_params=pltpu.CompilerParams(vmem_limit_bytes=48 * 1024 * 1024),
        name="experts",
        cost_estimate=pl.CostEstimate(
            flops=6 * count * width * units,
            bytes_accessed=6 * width * units + 4 * count * width,
            transcendentals=count * units,
        ),
    )(rows, gate_weight, up_weight, down_weight)


def shards(
    resid,
    queries,
    keys,
    values,
    forget_cache,
    query_gain,
    key_gain,
    out_weight,
    norm_gain,
    routes,
    group_weight,
    inner_share,
    expert_gate,
    expert_up,
    expert_down,
):
    dp_size = lax.axis_size("dp")
    sp_size = lax.axis_size("sp")
    tokens = queries.shape[1]
    head_size = query_gain.shape[0]
    local_heads = forget_cache.shape[1]
    local_width = local_heads * head_size
    lanes = LANES if local_width % LANES == 0 else local_width
    chunks = local_width // lanes
    packed = lanes // head_size
    sends = pack_heads(queries[0], keys[0], values[0], sp_size, chunks, lanes)
    arrived_qkv = [
        lax.all_to_all(send, SEQ, split_axis=0, concat_axis=0, tiled=True) for send in sends
    ]
    weight_shards = gather_start(out_weight, "dp")
    gains = jnp.stack([jnp.tile(query_gain, packed), jnp.tile(key_gain, packed)])
    level = forget_cache[0]
    level_columns = level.T
    returned_heads = []
    blocks = []
    for chunk in range(chunks):
        first = chunk * packed
        block = attend(
            arrived_qkv[chunk],
            gains,
            level[first : first + packed],
            level_columns[:, first : first + packed],
            tokens,
            head_size,
        )
        blocks.append(block)
        returned_heads.append(
            lax.all_to_all(
                block.reshape(sp_size, tokens, lanes),
                SEQ,
                split_axis=0,
                concat_axis=0,
                tiled=True,
            )
        )
    weight_shards = gather_rest(weight_shards, "dp", blocks)
    token_attn = (
        jnp.stack(returned_heads, axis=1)
        .transpose(2, 0, 1, 3)
        .reshape(tokens, sp_size * local_width)
    )
    pieces = [
        jnp.dot(token_attn, shard, preferred_element_type=jnp.float32) for shard in weight_shards
    ]
    pieces = order_pieces(pieces, "dp")
    projected = jnp.concatenate(pieces, axis=1)
    mid = (resid[0].astype(jnp.float32) + projected).astype(jnp.bfloat16)
    normed = norm_rows(mid, norm_gain)
    width = normed.shape[1]
    tok_count = normed.shape[0]
    top_count = routes.shape[2]
    experts = lax.axis_size("sp") * lax.axis_size("dp")
    capacity = 2 * tok_count * top_count // experts
    expert_ids = routes[0].reshape(-1)
    expert_onehot = (expert_ids[:, None] == jnp.arange(experts, dtype=jnp.int32)[None, :]).astype(
        jnp.int32
    )
    earlier = jnp.cumsum(expert_onehot, axis=0) - expert_onehot
    slot_rank = jnp.sum(earlier * expert_onehot, axis=1)
    slot_index = (expert_ids * capacity + slot_rank).reshape(tok_count, top_count)
    slot_range = jnp.arange(experts * capacity, dtype=jnp.int32)
    dispatch = jnp.any(slot_range[:, None, None] == slot_index[None, :, :], axis=2).astype(
        jnp.bfloat16
    )
    send = jnp.dot(dispatch, normed, preferred_element_type=jnp.float32).astype(jnp.bfloat16)
    arrived = lax.all_to_all(
        send.reshape(experts, capacity, width),
        ("sp", "dp"),
        split_axis=0,
        concat_axis=0,
        tiled=True,
    )
    flat_rows = arrived.reshape(-1, width)
    result = expert_of(flat_rows, expert_gate[0], expert_up[0], expert_down[0])
    returned = lax.all_to_all(
        result.reshape(arrived.shape), ("sp", "dp"), split_axis=0, concat_axis=0, tiled=True
    )
    returned = returned.reshape(experts * capacity, width)
    shares = inner_share[0]
    weights = group_weight[0][:, None] * shares / jnp.sum(shares, axis=-1, keepdims=True)
    mixed = jnp.zeros((tok_count, width), jnp.float32)
    for route in range(top_count):
        select = (slot_range[None, :] == slot_index[:, route : route + 1]).astype(jnp.bfloat16)
        picked = jnp.dot(select, returned, preferred_element_type=jnp.float32)
        mixed = mixed + weights[:, route : route + 1] * picked
    layer_out = (mid.astype(jnp.float32) + mixed).astype(jnp.bfloat16)
    return layer_out.reshape(1, tok_count, width)


def solution(mesh):
    return jax.shard_map(
        shards,
        mesh=mesh,
        in_specs=(
            P("dp", "sp", None),
            P("dp", "sp", None),
            P("dp", "sp", None),
            P("dp", "sp", None),
            P("dp", "sp", None),
            P(),
            P(),
            P(None, "dp"),
            P(),
            P("dp", "sp", None),
            P("dp", "sp"),
            P("dp", "sp", None),
            P(("sp", "dp"), None, None),
            P(("sp", "dp"), None, None),
            P(("sp", "dp"), None, None),
        ),
        out_specs=P("dp", "sp", None),
        check_vma=False,
    )
```
